32 devices in a mesh: sp: 4 (over x, core), dp: 8 (over z, y).
Axes of the slice: x: 2, y: 2, z: 4, core: 2. Of those that a mesh axis runs over, the one named last changes fastest.
Arguments:
- content_features_raw: bfloat16 [8, 512, 3072], P('dp', 'sp'), may hold values from -6 to 6
- memory_entering_matrix: bfloat16 [8, 512, 2048], P('dp', 'sp'), may hold values from -6 to 6
- memory_leaving_matrix: bfloat16 [8, 512, 2048], P('dp', 'sp'), may hold values from -6 to 6
- feature_switch_signal: bfloat16 [8, 512, 3072], P('dp', 'sp'), may hold values from -6 to 6
- ahead_increment_raw: float32 [8, 512, 48], P('dp', 'sp'), may hold values from -5 to 5
- reverse_increment_raw: float32 [8, 512, 48], P('dp', 'sp'), may hold values from -5 to 5
- additional_fading: float32 [8, 512, 48], P('dp', 'sp'), as said below
- content_filter_weights: bfloat16 [4, 3072], P(None, 'sp'), may hold values from -3 to 3
- entering_filter_weights: bfloat16 [4, 2048], P(None, 'sp'), may hold values from -3 to 3
- leaving_filter_weights: bfloat16 [4, 2048], P(None, 'sp'), may hold values from -3 to 3
- increment_offset_lanes: float32 [2, 48], P(None, 'sp'), may hold values from -0.5 to 0.5
- fading_speed_exponents: float32 [2, 48], P(None, 'sp'), as said below
- result_scaling_factor: bfloat16 [3072], replicated, may hold values from 0.099609375 to 1.8984375
Outputs:
- out: bfloat16 [8, 512, 3072], P('dp', 'sp')
The draws below stay inside these ranges and needn't reach their ends.
Inputs may be any that keep to these rules, and one draw needn't show every extreme that they name: Each head's row has a rate exp(fading_speed_exponents) between 0.3 / 4096 and 0.05. `additional_fading`: zero at most positions; elsewhere between log(0.5) and log(0.8).
All inputs are finite; a program needn't handle non-finite values.
Results may differ from the reference program's by a relative error of at most 0.0051.
Values may be sent and summed in bfloat16 or wider, within the bound.
A program may use at most 64 MiB of HBM per device.

```python
import math
import jax
import jax.numpy as jnp
from jax import lax

ATTENTION_LANES = 48
HEAD_DIM = 64
GROUPS = 16
STATE = 128
TAPS = 4
BLK = 128
TOK_DEV = 128
SEGMENTS = 8
SEG_LEN = 512
SEQ_LEN = 4096
D_SSM = 3072


def draw_fading_speed_exponents(key, part):
    first_key, second_key, third_key = jax.random.split(key, 3)
    share = 0.5
    slow_pick = jax.random.uniform(first_key, (2, ATTENTION_LANES), jnp.float32) < share
    slow_low = math.log(0.3 / SEQ_LEN)
    slow_high = math.log(min(2.0 / SEG_LEN, 0.015))
    slow_rate = jax.random.uniform(second_key, (2, ATTENTION_LANES), jnp.float32, slow_low, slow_high)
    fast_rate = jax.random.uniform(third_key, (2, ATTENTION_LANES), jnp.float32, math.log(0.015), math.log(0.05))
    return jnp.where(slow_pick, slow_rate, fast_rate).astype(jnp.float32)


def step_rates(key, salt):
    folded = jax.random.fold_in(key, salt)
    first_key, second_key = jax.random.split(folded)
    block_count = SEQ_LEN // TOK_DEV
    noise_draw = jnp.clip(jax.random.normal(first_key, (block_count, TOK_DEV, ATTENTION_LANES), jnp.float32), -3.0, 3.0)
    offset = jax.random.uniform(second_key, (block_count, 1, ATTENTION_LANES), jnp.float32, -1.2, 1.2)
    return (noise_draw + offset).reshape(SEGMENTS, SEG_LEN, ATTENTION_LANES).astype(jnp.float32)


def draw_ahead_increment_raw(key, part):
    return step_rates(key, 11)


def draw_reverse_increment_raw(key, part):
    return step_rates(key, 23)


def draw_additional_fading(key, part):
    first_key, second_key = jax.random.split(key)
    struck = jax.random.uniform(first_key, (SEGMENTS, SEG_LEN, ATTENTION_LANES), jnp.float32) < 3.0 / SEQ_LEN
    loss_log = jnp.log(jax.random.uniform(second_key, (SEGMENTS, SEG_LEN, ATTENTION_LANES), jnp.float32, 0.5, 0.8))
    return jnp.where(struck, loss_log, 0.0).astype(jnp.float32)


def levels(rng, extent, cuts, low, largest):
    def one(position, shards_of):
        steps = jax.random.uniform(jax.random.fold_in(jax.random.fold_in(rng, 6), position), (shards_of,), jnp.float32, low / len(cuts), largest / len(cuts))
        return jnp.repeat(jnp.exp(steps), extent[position] // shards_of).reshape((-1,) + (1,) * (len(extent) - position - 1))

    level = one(*cuts[0])
    for cut in cuts[1:]:
        level = level * one(*cut)
    return level


def gaussian(stream_key, extent, spread, limit, shards=(), kind=jnp.bfloat16):
    values = jax.random.normal(stream_key, extent, jnp.float32) * spread
    if len(shards) > 0:
        values = levels(stream_key, extent, shards, -0.22, 0.18) * values
    return jnp.clip(values, min=-limit, max=limit).astype(kind)


def setup_inputs(seed: int = 0) -> dict:
    streams_of = jax.random.split(jax.random.key(seed), 14)
    content_features_raw = gaussian(streams_of[0], (SEGMENTS, SEG_LEN, D_SSM), 1.0, 6.0, ((0, 8), (1, 4)))
    memory_entering_matrix = gaussian(streams_of[1], (SEGMENTS, SEG_LEN, GROUPS * STATE), 1.0, 6.0, ((0, 8), (1, 4)))
    memory_leaving_matrix = gaussian(streams_of[2], (SEGMENTS, SEG_LEN, GROUPS * STATE), 1.0, 6.0, ((0, 8), (1, 4)))
    feature_switch_signal = gaussian(streams_of[3], (SEGMENTS, SEG_LEN, D_SSM), 1.0, 6.0, ((0, 8), (1, 4)))
    ahead_increment_raw = draw_ahead_increment_raw(jax.random.fold_in(streams_of[13], 71), 0)
    reverse_increment_raw = draw_reverse_increment_raw(jax.random.fold_in(streams_of[13], 71), 0)
    additional_fading = draw_additional_fading(jax.random.fold_in(streams_of[13], 71), 0)
    content_filter_weights = gaussian(streams_of[7], (TAPS, D_SSM), TAPS ** -0.5, 3.0, ((1, 4),))
    entering_filter_weights = gaussian(streams_of[8], (TAPS, GROUPS * STATE), TAPS ** -0.5, 3.0, ((1, 4),))
    leaving_filter_weights = gaussian(streams_of[9], (TAPS, GROUPS * STATE), TAPS ** -0.5, 3.0, ((1, 4),))
    increment_offset_lanes = jnp.clip(jax.random.uniform(streams_of[10], (2, ATTENTION_LANES), jnp.float32, -0.5, 0.5) * levels(streams_of[10], (2, ATTENTION_LANES), ((1, 4),), -0.4, 0.0), -0.5, 0.5)
    fading_speed_exponents = draw_fading_speed_exponents(jax.random.fold_in(streams_of[13], 71), 0)
    result_scaling_factor = jnp.clip(1.0 + 0.18 * jax.random.normal(streams_of[12], (D_SSM,), jnp.float32), 0.099609375, 1.8984375).astype(jnp.bfloat16)
    return {"content_features_raw": content_features_raw, "memory_entering_matrix": memory_entering_matrix, "memory_leaving_matrix": memory_leaving_matrix, "feature_switch_signal": feature_switch_signal, "ahead_increment_raw": ahead_increment_raw, "reverse_increment_raw": reverse_increment_raw, "additional_fading": additional_fading, "content_filter_weights": content_filter_weights, "entering_filter_weights": entering_filter_weights, "leaving_filter_weights": leaving_filter_weights, "increment_offset_lanes": increment_offset_lanes, "fading_speed_exponents": fading_speed_exponents, "result_scaling_factor": result_scaling_factor}


def conv_silu(padded, weight, length):
    total_sum = padded[0:length].astype(jnp.float32) * weight[0].astype(jnp.float32)
    for lag_step in range(1, weight.shape[0]):
        total_sum = total_sum + padded[lag_step:lag_step + length].astype(jnp.float32) * weight[lag_step].astype(jnp.float32)
    return jax.nn.silu(total_sum).astype(jnp.bfloat16)

def direction(x_conv, b_conv, c_conv, rate, log_decay):
    overall_position_count = x_conv.shape[0]
    heads_within_group = rate.shape[1]
    block_count = overall_position_count // BLK
    x_blocks = x_conv.reshape(block_count, BLK, heads_within_group, HEAD_DIM)
    b_blocks = b_conv.reshape(block_count, BLK, STATE)
    c_blocks = c_conv.reshape(block_count, BLK, STATE)
    rate_blocks = rate.reshape(block_count, BLK, heads_within_group)
    log_blocks = log_decay.reshape(block_count, BLK, heads_within_group)
    lower_mask = jnp.tril(jnp.ones((BLK, BLK), bool))[:, :, None]

    def step(state, pieces):
        x_block, b_block, c_block, rate_block, log_block = pieces
        cum_log = jnp.cumsum(log_block, axis=0)
        scores = jnp.dot(c_block, b_block.T, preferred_element_type=jnp.float32)
        log_gaps = jnp.where(lower_mask, cum_log[:, None, :] - cum_log[None, :, :], -jnp.inf)
        weights = (scores[:, :, None] * jnp.exp(log_gaps) * rate_block[None, :, :]).astype(jnp.bfloat16)
        local_part = jnp.einsum('lsh,shp->lhp', weights.astype(jnp.float32), x_block.astype(jnp.float32))
        carried_part = jnp.einsum('ln,hpn->lhp', c_block.astype(jnp.float32), state, precision=lax.Precision.HIGHEST) * jnp.exp(cum_log)[:, :, None]
        block_log = cum_log[-1]
        scaled = (x_block.astype(jnp.float32) * (rate_block * jnp.exp(block_log[None, :] - cum_log))[:, :, None]).astype(jnp.bfloat16)
        update = jnp.einsum('shp,sn->hpn', scaled.astype(jnp.float32), b_block.astype(jnp.float32))
        new_state = state * jnp.exp(block_log)[:, None, None] + update
        return (new_state, local_part + carried_part)
    initial = jnp.zeros((heads_within_group, HEAD_DIM, STATE), jnp.float32)
    _, outputs = lax.scan(step, initial, (x_blocks, b_blocks, c_blocks, rate_blocks, log_blocks))
    return outputs.reshape(overall_position_count, heads_within_group * HEAD_DIM)

def reference(content_features_raw, memory_entering_matrix, memory_leaving_matrix, feature_switch_signal, ahead_increment_raw, reverse_increment_raw, additional_fading, content_filter_weights, entering_filter_weights, leaving_filter_weights, increment_offset_lanes, fading_speed_exponents, result_scaling_factor):
    overall_position_count = SEGMENTS * SEG_LEN
    width = ATTENTION_LANES * HEAD_DIM
    heads_within_group = ATTENTION_LANES // GROUPS
    group_width = heads_within_group * HEAD_DIM
    x_flat = content_features_raw.reshape(overall_position_count, width)
    b_flat = memory_entering_matrix.reshape(overall_position_count, GROUPS * STATE)
    c_flat = memory_leaving_matrix.reshape(overall_position_count, GROUPS * STATE)
    z_flat = feature_switch_signal.reshape(overall_position_count, width)
    fwd_flat = ahead_increment_raw.reshape(overall_position_count, ATTENTION_LANES)
    bwd_flat = reverse_increment_raw.reshape(overall_position_count, ATTENTION_LANES)
    additional_fading_flat_array = additional_fading.reshape(overall_position_count, ATTENTION_LANES)

    def one_group(group):
        col_x = (group * group_width).astype(jnp.int32)
        col_b = (group * STATE).astype(jnp.int32)
        column_per_head = (group * heads_within_group).astype(jnp.int32)
        x_part = lax.dynamic_slice_in_dim(x_flat, col_x, group_width, 1)
        b_part = lax.dynamic_slice_in_dim(b_flat, col_b, STATE, 1)
        c_part = lax.dynamic_slice_in_dim(c_flat, col_b, STATE, 1)
        z_part = lax.dynamic_slice_in_dim(z_flat, col_x, group_width, 1)
        pad_rows = ((2, TAPS - 3), (0, 0))
        x_conv = conv_silu(jnp.pad(x_part, pad_rows), lax.dynamic_slice_in_dim(content_filter_weights, col_x, group_width, 1), overall_position_count)
        b_conv = conv_silu(jnp.pad(b_part, pad_rows), lax.dynamic_slice_in_dim(entering_filter_weights, col_b, STATE, 1), overall_position_count)
        c_conv = conv_silu(jnp.pad(c_part, pad_rows), lax.dynamic_slice_in_dim(leaving_filter_weights, col_b, STATE, 1), overall_position_count)
        bias_part = lax.dynamic_slice_in_dim(increment_offset_lanes, column_per_head, heads_within_group, 1)
        decay_log_piece = lax.dynamic_slice_in_dim(fading_speed_exponents, column_per_head, heads_within_group, 1)
        spike_piece = lax.dynamic_slice_in_dim(additional_fading_flat_array, column_per_head, heads_within_group, 1)
        forward_step_rate = jax.nn.softplus(lax.dynamic_slice_in_dim(fwd_flat, column_per_head, heads_within_group, 1) + bias_part[0])
        backward_step_rate = jax.nn.softplus(lax.dynamic_slice_in_dim(bwd_flat, column_per_head, heads_within_group, 1) + bias_part[1])
        forward_log_decay = -jnp.exp(decay_log_piece[0]) * forward_step_rate + spike_piece
        backward_log_decay = -jnp.exp(decay_log_piece[1]) * backward_step_rate + spike_piece
        y_fwd = direction(x_conv, b_conv, c_conv, forward_step_rate, forward_log_decay)
        y_bwd = direction(x_conv[::-1], b_conv[::-1], c_conv[::-1], backward_step_rate[::-1], backward_log_decay[::-1])[::-1]
        mixed = (y_fwd + y_bwd).astype(jnp.bfloat16)
        gated = mixed.astype(jnp.float32) * jax.nn.silu(z_part.astype(jnp.float32))
        by_head = gated.reshape(overall_position_count, heads_within_group, HEAD_DIM)
        normed = by_head * lax.rsqrt(lax.optimization_barrier(jnp.mean(by_head * by_head, axis=-1, keepdims=True)) + 1e-06)
        gain_part = lax.dynamic_slice_in_dim(result_scaling_factor, col_x, group_width, 0).astype(jnp.float32)
        return (normed.reshape(overall_position_count, group_width) * gain_part).astype(jnp.bfloat16)
    results = lax.map(one_group, jnp.arange(GROUPS, dtype=jnp.int32))
    return jnp.transpose(results, (1, 0, 2)).reshape(SEGMENTS, SEG_LEN, width)
```

```python
import functools

import jax
import jax.numpy as jnp
from jax import lax
from jax.experimental import pallas as pl
from jax.experimental.pallas import tpu as pltpu
from jax.sharding import PartitionSpec as P

F32 = jnp.float32
BF16 = jnp.bfloat16
HEAD_DIM = 64
STATE = 128
HIGHEST = lax.Precision.HIGHEST


def levels_of(sp, dp, groups):
    found = []
    split = 1
    core = 2 if sp % 2 == 0 else 1
    inner = 2 if dp % 2 == 0 and groups % (2 * sp) == 0 else 1
    for axis, count, stride in (("sp", core, 1), ("sp", sp // core, core), ("dp", inner, 1)):
        if count > 1:
            found.append((axis, count, stride))
            split *= count
    return tuple(found), ("dp", dp // inner, inner)


def digit_of(level):
    axis, count, stride = level
    return lax.rem(lax.axis_index(axis) // stride, count)


def member_id(level, member):
    axis, count, stride = level
    return {axis: lax.axis_index(axis) + (member - digit_of(level)) * stride}


def kernel(levels, top, sizes, *refs):
    heads, pairs = sizes
    (x_ref, b_ref, c_ref, z_ref, inc_ref, spike_ref, prm_ref, w_ref, halo_ref, gain_ref) = refs[:10]
    out_ref = refs[10]
    (xc, bc, cc, y_ref, cum_ref, rate_ref, cum_t, rate_t, fac_ref, first_total, first_log) = refs[11:22]
    rest = list(refs[22:])
    up, up_log, down, stage, totals, logs, sems = [], [], [], [], [first_total], [first_log], []
    for _ in levels:
        up.append(rest.pop(0))
        up_log.append(rest.pop(0))
        down.append(rest.pop(0))
        stage.append(rest.pop(0))
        totals.append(rest.pop(0))
        logs.append(rest.pop(0))
        sems.append(rest.pop(0))
    top_in, top_log, top_sem, incoming, decay = rest
    blk = x_ref.shape[0]
    per_pair = heads // pairs
    x_w = per_pair * HEAD_DIM
    b_w = 2 * STATE
    tiles = x_w // 128
    lane = lax.broadcasted_iota(jnp.int32, (blk, 128), 1)
    left = lane < HEAD_DIM
    row = lax.broadcasted_iota(jnp.int32, (blk, 128), 0)

    barrier = pltpu.get_barrier_semaphore()
    greeted = 0
    for level in levels + (top,):
        me = digit_of(level)
        for o in range(1, level[1]):
            pl.semaphore_signal(
                barrier,
                inc=1,
                device_id=member_id(level, lax.rem(me + o, level[1])),
                device_id_type=pl.DeviceIdType.MESH,
            )
            greeted += 1

    rate = jax.nn.softplus(inc_ref[...] + prm_ref[0:1, :])
    log_decay = -jnp.exp(prm_ref[1:2, :]) * rate + spike_ref[...]
    lower = (lane <= row).astype(F32)
    upper = (lane >= row).astype(F32)
    cum_f = jnp.dot(lower, log_decay, precision=HIGHEST, preferred_element_type=F32)
    cum_b = jnp.dot(upper, log_decay, precision=HIGHEST, preferred_element_type=F32)
    cum = jnp.where(lane < heads, cum_f, cum_b)
    lane1 = lane[0:1]
    last = jnp.where(lane1 < heads, cum_f[blk - 1 : blk], cum_b[0:1])
    cum_ref[...] = cum
    rate_ref[...] = rate
    cum_t[...] = cum.T
    rate_t[...] = rate.T
    fac_ref[...] = rate * jnp.exp(last - cum)
    first_log[...] = jnp.broadcast_to(last, (8, 128))

    def rolled(ref, p):
        return pltpu.roll(ref[...], lax.rem(128 - p * per_pair, 128), 1)

    def two(cols, i):
        return jnp.where(left, cols[:, i : i + 1], cols[:, i + 1 : i + 2])

    def conv(src, col, width, off):
        at = pl.ds(pl.multiple_of(off + col, 128), width)
        v = src[:, pl.ds(pl.multiple_of(col, 128), width)].astype(F32)
        r = lax.broadcasted_iota(jnp.int32, (blk, width), 0)
        h0, h1, h2 = halo_ref[0:1, at], halo_ref[1:2, at], halo_ref[2:3, at]
        m1 = jnp.where(r == 0, h1, pltpu.roll(v, 1, 0))
        m2 = jnp.where(r == 0, h0, jnp.where(r == 1, h1, pltpu.roll(v, 2, 0)))
        p1 = jnp.where(r == blk - 1, h2, pltpu.roll(v, blk - 1, 0))
        s = m2 * w_ref[0:1, at] + m1 * w_ref[1:2, at] + v * w_ref[2:3, at] + p1 * w_ref[3:4, at]
        return (s / (1.0 + jnp.exp(-s))).astype(BF16)

    x_total = x_ref.shape[1]
    b_total = b_ref.shape[1]

    def first(p, _):
        x_at = pl.ds(pl.multiple_of(p * x_w, 128), x_w)
        b_at = pl.ds(pl.multiple_of(p * b_w, 128), b_w)
        xv = conv(x_ref, p * x_w, x_w, 0)
        bv = conv(b_ref, p * b_w, b_w, x_total)
        xc[:, x_at] = xv
        bc[:, b_at] = bv
        cc[:, b_at] = conv(c_ref, p * b_w, b_w, x_total + b_total)
        cols = rolled(fac_ref, p)
        xf = xv.astype(F32)
        for d in range(2):
            scaled = jnp.concatenate(
                [
                    (xf[:, k * 128 : (k + 1) * 128] * two(cols, d * heads + 2 * k)).astype(BF16)
                    for k in range(tiles)
                ],
                axis=1,
            )
            u = lax.dot_general(scaled, bv, (((0,), (0,)), ((), ())), preferred_element_type=F32)
            half = x_w // 2
            rows = pl.ds(pl.multiple_of(p * x_w, 128), x_w)
            first_total[d, rows, :] = jnp.concatenate(
                [u[:half, :STATE], u[half:, STATE:]], axis=0
            ).astype(BF16)
        return 0

    lax.fori_loop(0, pairs, first, 0)
    pl.semaphore_wait(barrier, greeted)

    def inner(p, _):
        x_at = pl.ds(pl.multiple_of(p * x_w, 128), x_w)
        b_at = pl.ds(pl.multiple_of(p * b_w, 128), b_w)
        bv, cv, xv = bc[:, b_at], cc[:, b_at], xc[:, x_at]
        cols = rolled(cum_ref, p)
        parts = []
        for g in range(2):
            scores = lax.dot_general(
                cv[:, g * STATE : (g + 1) * STATE],
                bv[:, g * STATE : (g + 1) * STATE],
                (((1,), (1,)), ((), ())),
                preferred_element_type=F32,
            )
            for i in range(per_pair // 2):
                h = g * (per_pair // 2) + i
                hf = p * per_pair + h
                gap_f = cols[:, h : h + 1] - cum_t[pl.ds(hf, 1), :]
                gap_b = cols[:, heads + h : heads + h + 1] - cum_t[pl.ds(heads + hf, 1), :]
                gap = jnp.where(lane < row, gap_f, jnp.where(lane > row, gap_b, 0.0))
                rf, rb = rate_t[pl.ds(hf, 1), :], rate_t[pl.ds(heads + hf, 1), :]
                scale = jnp.where(lane < row, rf, jnp.where(lane > row, rb, rf + rb))
                parts.append((scores * jnp.exp(gap) * scale).astype(BF16))
        for k in range(tiles):
            xt = xv[:, k * 128 : (k + 1) * 128]
            zero = jnp.zeros_like(xt)
            both = jnp.concatenate([jnp.where(left, xt, zero), jnp.where(left, zero, xt)], axis=0)
            w = jnp.concatenate([parts[2 * k], parts[2 * k + 1]], axis=1)
            y_ref[:, pl.ds(pl.multiple_of(p * x_w + k * 128, 128), 128)] = jnp.dot(
                w, both, preferred_element_type=F32
            )
        return 0

    def copy(src, dst, send, recv, level, member):
        return pltpu.make_async_remote_copy(
            src_ref=src,
            dst_ref=dst,
            send_sem=send,
            recv_sem=recv,
            device_id=member_id(level, member),
            device_id_type=pl.DeviceIdType.MESH,
        )

    def expand(slot, tile):
        decay[slot] = jnp.exp(jnp.broadcast_to(tile[0:1, :], (128, 128)).T)

    slots = len(levels) + 1
    cuts = [(i * pairs) // slots for i in range(slots + 1)]
    base = jnp.int32(0)
    bases = []
    for k, level in enumerate(levels):
        n = level[1]
        me = digit_of(level)
        total, log = totals[k], logs[k]
        rows = total.shape[1] // n
        sem = sems[k]
        pending = []
        for o in range(1, n):
            m = lax.rem(me + o, n)
            part = total.at[:, pl.ds(pl.multiple_of(m * rows, 64), rows), :]
            pending.append(copy(part, up[k].at[me], sem.at[0, m], sem.at[1, me], level, m))
            pending.append(copy(log, up_log[k].at[me], sem.at[2, m], sem.at[3, me], level, m))
        for one in pending:
            one.start()
        up[k][me] = total[:, pl.ds(pl.multiple_of(me * rows, 64), rows), :]
        up_log[k][me] = log[...]
        lax.fori_loop(cuts[k], cuts[k + 1], inner, 0)
        for one in pending:
            one.wait_send()
        for o in range(1, n):
            s = lax.rem(me + o, n)
            part = total.at[:, pl.ds(0, rows), :]
            copy(part, up[k].at[s], sem.at[0, s], sem.at[1, s], level, s).wait_recv()
            copy(log, up_log[k].at[s], sem.at[2, s], sem.at[3, s], level, s).wait_recv()
        base = base + me * (rows // HEAD_DIM)
        bases.append(base)
        log_sum = up_log[k][0]
        for m in range(1, n):
            log_sum = log_sum + up_log[k][m]
        logs[k + 1][...] = log_sum
        for m in range(n):
            expand(m, up_log[k][m])

        def gather(h, _, k=k, n=n, base=base):
            at = pl.ds(pl.multiple_of(h * HEAD_DIM, HEAD_DIM), HEAD_DIM)
            f = up[k][0, 0, at, :].astype(F32)
            b = up[k][n - 1, 1, at, :].astype(F32)
            for m in range(1, n):
                f = f * decay[m, pl.ds(base + h, 1), :] + up[k][m, 0, at, :].astype(F32)
                r = n - 1 - m
                b = b * decay[r, pl.ds(heads + base + h, 1), :] + up[k][r, 1, at, :].astype(F32)
            totals[k + 1][0, at, :] = f.astype(BF16)
            totals[k + 1][1, at, :] = b.astype(BF16)
            return 0

        lax.fori_loop(0, rows // HEAD_DIM, gather, 0)

    n = top[1]
    me = digit_of(top)
    total, log = totals[-1], logs[-1]
    pending = []
    for o in range(1, n):
        m = lax.rem(me + o, n)
        d = jnp.where(m < me, 1, 0)
        pending.append(
            copy(total.at[d], top_in.at[me], top_sem.at[0, m], top_sem.at[1, me], top, m)
        )
        pending.append(copy(log, top_log.at[me], top_sem.at[2, m], top_sem.at[3, me], top, m))
    for one in pending:
        one.start()
    lax.fori_loop(cuts[-2], cuts[-1], inner, 0)
    for one in pending:
        one.wait_send()
    for o in range(1, n):
        s = lax.rem(me + o, n)
        copy(total.at[0], top_in.at[s], top_sem.at[0, s], top_sem.at[1, s], top, s).wait_recv()
        copy(log, top_log.at[s], top_sem.at[2, s], top_sem.at[3, s], top, s).wait_recv()
    incoming[...] = jnp.zeros_like(incoming)

    def carry(s, d):
        expand(0, top_log[s])

        def one_head(h, _):
            at = pl.ds(pl.multiple_of(h * HEAD_DIM, HEAD_DIM), HEAD_DIM)
            factor = decay[0, pl.ds(d * heads + base + h, 1), :]
            incoming[d, at, :] = incoming[d, at, :] * factor + top_in[s, at, :].astype(F32)
            return 0

        lax.fori_loop(0, total.shape[1] // HEAD_DIM, one_head, 0)
        return 0

    lax.fori_loop(0, me, lambda s, _: carry(s, 0), 0)
    lax.fori_loop(0, n - 1 - me, lambda i, _: carry(n - 1 - i, 1), 0)

    for k in reversed(range(len(levels))):
        level = levels[k]
        n = level[1]
        me = digit_of(level)
        sem = sems[k]
        rows = totals[k].shape[1] // n
        source = incoming if k == len(levels) - 1 else down[k + 1]
        for m in range(n):
            expand(m, up_log[k][m])

        def spread(h, _, k=k, n=n, base=bases[k], source=source):
            at = pl.ds(pl.multiple_of(h * HEAD_DIM, HEAD_DIM), HEAD_DIM)
            f = source[0, at, :].astype(F32)
            b = source[1, at, :].astype(F32)
            for m in range(n):
                r = n - 1 - m
                stage[k][m, 0, at, :] = f.astype(BF16)
                stage[k][r, 1, at, :] = b.astype(BF16)
                if m < n - 1:
                    f = f * decay[m, pl.ds(base + h, 1), :] + up[k][m, 0, at, :].astype(F32)
                    b = b * decay[r, pl.ds(heads + base + h, 1), :] + up[k][r, 1, at, :].astype(F32)
            return 0

        lax.fori_loop(0, rows // HEAD_DIM, spread, 0)
        mine = pl.ds(pl.multiple_of(me * rows, 64), rows)
        pending = []
        for o in range(1, n):
            m = lax.rem(me + o, n)
            pending.append(
                copy(stage[k].at[m], down[k].at[:, mine, :], sem.at[4, m], sem.at[5, me], level, m)
            )
        for one in pending:
            one.start()
        down[k][:, mine, :] = stage[k][me]
        for one in pending:
            one.wait_send()
        for o in range(1, n):
            s = lax.rem(me + o, n)
            theirs = pl.ds(pl.multiple_of(s * rows, 64), rows)
            copy(
                stage[k].at[s], down[k].at[:, theirs, :], sem.at[4, s], sem.at[5, s], level, s
            ).wait_recv()

    final = down[0] if levels else incoming
    cum_ref[...] = jnp.exp(cum_ref[...])

    def last_part(p, _):
        x_at = pl.ds(pl.multiple_of(p * x_w, 128), x_w)
        cv = cc[:, pl.ds(pl.multiple_of(p * b_w, 128), b_w)]
        cols = rolled(cum_ref, p)
        carried = []
        for d in range(2):
            st = final[d, x_at, :].astype(BF16)
            got = [
                lax.dot_general(
                    cv[:, g * STATE : (g + 1) * STATE],
                    st,
                    (((1,), (1,)), ((), ())),
                    preferred_element_type=F32,
                )
                for g in range(2)
            ]
            carried.append(got)
        for k in range(tiles):
            cut = slice(k * 128, (k + 1) * 128)
            at = pl.ds(pl.multiple_of(p * x_w + k * 128, 128), 128)
            y = y_ref[:, at]
            for d in range(2):
                a, b = carried[d][0][:, cut], carried[d][1][:, cut]
                if 2 * k + 1 < per_pair // 2:
                    v = a
                elif 2 * k >= per_pair // 2:
                    v = b
                else:
                    v = jnp.where(left, a, b)
                y = y + v * two(cols, d * heads + 2 * k)
            z = z_ref[:, at].astype(F32)
            gated = y.astype(BF16).astype(F32) * (z / (1.0 + jnp.exp(-z)))
            square = gated * gated
            low = jnp.sum(jnp.where(left, square, 0.0), axis=1, keepdims=True)
            high = jnp.sum(jnp.where(left, 0.0, square), axis=1, keepdims=True)
            mean = jnp.where(left, low, high) * (1.0 / HEAD_DIM)
            out_ref[:, at] = (gated * lax.rsqrt(mean + 1e-6) * gain_ref[0:1, at]).astype(BF16)
        return 0

    lax.fori_loop(0, pairs, last_part, 0)


def local(sp, dp, x, b, c, z, ahead, back, spike, wx, wb, wc, offset, fading, gain):
    x, b, c, z = x[0], b[0], c[0], z[0]
    blk, x_total = x.shape
    groups = b.shape[1] // STATE
    heads = ahead.shape[2]
    pairs = groups // 2
    xw, bw, hw = wx.shape[1], wb.shape[1], offset.shape[1]
    taps = jnp.concatenate([wx, wb, wc], axis=1).astype(F32)
    small = jnp.concatenate([offset, fading], axis=0)
    packed = jnp.concatenate([taps, jnp.pad(small, ((0, 0), (0, taps.shape[1] - hw)))], axis=0)
    every = lax.all_gather(packed, "sp")
    whole = jnp.transpose(every, (1, 0, 2))
    w = jnp.concatenate(
        [
            whole[:, :, :xw].reshape(8, -1),
            whole[:, :, xw : xw + bw].reshape(8, -1),
            whole[:, :, xw + bw :].reshape(8, -1),
        ],
        axis=1,
    )
    tail = jnp.zeros((128 - 2 * heads,), F32)
    flat = whole[4:8, :, :hw].reshape(4, heads)
    prm = jnp.stack(
        [jnp.concatenate([flat[0], flat[1], tail]), jnp.concatenate([flat[2], flat[3], tail])]
    )
    prm = jnp.pad(prm, ((0, 6), (0, 0)))
    count = sp * dp
    place = [(i % sp) * dp + i // sp for i in range(count)]
    ring = list(zip(place[:-1], place[1:]))
    edge = jnp.concatenate([x[-2:], b[-2:], c[-2:]], axis=1)
    head = jnp.concatenate([x[:1], b[:1], c[:1]], axis=1)
    before = lax.ppermute(edge, ("sp", "dp"), ring)
    after = lax.ppermute(head, ("sp", "dp"), [(j, i) for i, j in ring])
    halo = jnp.pad(jnp.concatenate([before, after], axis=0).astype(F32), ((0, 5), (0, 0)))
    pad = jnp.zeros((blk, 128 - 2 * heads), F32)
    inc = jnp.concatenate([ahead[0], back[0], pad], axis=1)
    spikes = jnp.concatenate([spike[0], spike[0], pad], axis=1)

    levels, top = levels_of(sp, dp, groups)
    scratch = [
        pltpu.VMEM((blk, x_total), BF16),
        pltpu.VMEM((blk, groups * STATE), BF16),
        pltpu.VMEM((blk, groups * STATE), BF16),
        pltpu.VMEM((blk, x_total), F32),
    ]
    scratch += [pltpu.VMEM((128, 128), F32)] * 5
    rows = x_total
    scratch += [pltpu.VMEM((2, rows, STATE), BF16), pltpu.VMEM((8, 128), F32)]
    widest = 1
    for _, n, _ in levels:
        widest = max(widest, n)
        scratch += [
            pltpu.VMEM((n, 2, rows // n, STATE), BF16),
            pltpu.VMEM((n, 8, 128), F32),
            pltpu.VMEM((2, rows, STATE), BF16),
            pltpu.VMEM((n, 2, rows // n, STATE), BF16),
            pltpu.VMEM((2, rows // n, STATE), BF16),
            pltpu.VMEM((8, 128), F32),
            pltpu.SemaphoreType.DMA((6, n)),
        ]
        rows //= n
    scratch += [
        pltpu.VMEM((top[1], rows, STATE), BF16),
        pltpu.VMEM((top[1], 8, 128), F32),
        pltpu.SemaphoreType.DMA((4, top[1])),
        pltpu.VMEM((2, rows, STATE), F32),
        pltpu.VMEM((widest, 128, 128), F32),
    ]
    out = pl.pallas_call(
        functools.partial(kernel, levels, top, (heads, pairs)),
        out_shape=jax.ShapeDtypeStruct((blk, x_total), BF16),
        in_specs=[pl.BlockSpec(memory_space=pltpu.VMEM)] * 10,
        out_specs=pl.BlockSpec(memory_space=pltpu.VMEM),
        scratch_shapes=scratch,
        compiler_params=pltpu.CompilerParams(
            collective_id=0, has_side_effects=True, vmem_limit_bytes=60 * 2**20
        ),
        name="mixer",
    )(x, b, c, z, inc, spikes, prm, w, halo, gain.astype(F32)[None])
    return out[None]


def solution(mesh):
    tokens = P("dp", "sp", None)
    placed = (tokens,) * 7 + (P(None, "sp"),) * 5 + (P(),)
    return jax.shard_map(
        functools.partial(local, mesh.shape["sp"], mesh.shape["dp"]),
        mesh=mesh,
        in_specs=placed,
        out_specs=tokens,
        check_vma=False,
    )
```

```python
import functools

import jax
import jax.numpy as jnp
from jax import lax
from jax.experimental import pallas as pl
from jax.experimental.pallas import tpu as pltpu
from jax.sharding import PartitionSpec as P

F32 = jnp.float32
BF16 = jnp.bfloat16
HEAD_DIM = 64
STATE = 128
EDGE = 8
HIGHEST = lax.Precision.HIGHEST


def levels_of(sp, dp, groups):
    found = []
    split = 1
    core = 2 if sp % 2 == 0 else 1
    inner = 2 if dp % 2 == 0 and groups % (2 * sp) == 0 else 1
    for axis, count, stride in (("sp", core, 1), ("sp", sp // core, core), ("dp", inner, 1)):
        if count > 1:
            found.append((axis, count, stride))
            split *= count
    return tuple(found), ("dp", dp // inner, inner)


def digit_of(level):
    axis, count, stride = level
    return lax.rem(lax.axis_index(axis) // stride, count)


def member_id(level, member):
    axis, count, stride = level
    return {axis: lax.axis_index(axis) + (member - digit_of(level)) * stride}


def kernel(levels, top, sizes, *refs):
    heads, pairs, sp, dp = sizes
    (x_ref, b_ref, c_ref, z_ref, ahead_ref, back_ref, spike_ref) = refs[:7]
    params = refs[7:12]
    gain_ref, out_ref = refs[12:14]
    (xc, bc, cc, y_ref, cum_ref, rate_ref, cum_t, rate_t, fac_ref, first_total, first_log) = refs[14:25]
    got, w_ref, prm_ref, halo_ref, edges, early_sem, edge_sem = (
        refs[25:30], refs[30], refs[31], refs[32], refs[33:39], refs[39], refs[40]
    )
    rest = list(refs[41:])
    up, up_log, down, stage, totals, logs, sems = [], [], [], [], [first_total], [first_log], []
    for _ in levels:
        up.append(rest.pop(0))
        up_log.append(rest.pop(0))
        down.append(rest.pop(0))
        stage.append(rest.pop(0))
        totals.append(rest.pop(0))
        logs.append(rest.pop(0))
        sems.append(rest.pop(0))
    top_in, top_log, top_sem, incoming, decay = rest
    blk = x_ref.shape[0]
    per_pair = heads // pairs
    x_w = per_pair * HEAD_DIM
    b_w = 2 * STATE
    tiles = x_w // 128
    lane = lax.broadcasted_iota(jnp.int32, (blk, 128), 1)
    left = lane < HEAD_DIM
    row = lax.broadcasted_iota(jnp.int32, (blk, 128), 0)

    segment = ("sp", sp, 1)
    here, there = lax.axis_index("sp"), lax.axis_index("dp")
    rank = there * sp + here
    has_next, has_prev = rank < sp * dp - 1, rank > 0
    after = {"sp": lax.rem(here + 1, sp), "dp": lax.rem(there + (here + 1) // sp, dp)}
    before = {
        "sp": lax.rem(here + sp - 1, sp),
        "dp": lax.rem(there + dp - (sp - here) // sp, dp),
    }
    mesh_id = pl.DeviceIdType.MESH
    barrier = pltpu.get_barrier_semaphore()
    greeted = 0
    for level in levels + (top, segment):
        me = digit_of(level)
        for o in range(1, level[1]):
            target = member_id(level, lax.rem(me + o, level[1]))
            pl.semaphore_signal(barrier, inc=1, device_id=target, device_id_type=mesh_id)
            greeted += 1
    for present, target in ((has_next, after), (has_prev, before)):

        @pl.when(present)
        def _(target=target):
            pl.semaphore_signal(barrier, inc=1, device_id=target, device_id_type=mesh_id)

    filler = jnp.zeros((128 - 2 * heads, blk), F32)
    inc = jnp.concatenate([ahead_ref[...], back_ref[...], filler], axis=0).T
    spikes = jnp.concatenate([spike_ref[...], spike_ref[...], filler], axis=0).T
    count = sp * dp
    neighbours = (rank + count - 1) // count + (2 * count - 2 - rank) // count
    pl.semaphore_wait(barrier, greeted + neighbours)

    def edge_copy(i, direction):
        src = (x_ref, b_ref, c_ref)[i]
        start = blk - EDGE if direction == 0 else 0
        return pltpu.make_async_remote_copy(
            src_ref=src.at[pl.ds(start, EDGE), :],
            dst_ref=edges[3 * direction + i],
            send_sem=edge_sem.at[0, direction, i],
            recv_sem=edge_sem.at[1, direction, i],
            device_id=(after, before)[direction],
            device_id_type=mesh_id,
        )

    def param_copy(i, member, slot):
        return pltpu.make_async_remote_copy(
            src_ref=params[i],
            dst_ref=got[i].at[slot],
            send_sem=early_sem.at[0, i, member],
            recv_sem=early_sem.at[1, i, slot],
            device_id=member_id(segment, member),
            device_id_type=mesh_id,
        )

    for o in range(1, sp):
        for i in range(5):
            param_copy(i, lax.rem(here + o, sp), here).start()
    for direction, present in ((0, has_next), (1, has_prev)):

        @pl.when(present)
        def _(direction=direction):
            for i in range(3):
                edge_copy(i, direction).start()

    for i in range(5):
        got[i][here] = params[i][...]
    for o in range(1, sp):
        for i in range(5):
            s = lax.rem(here + o, sp)
            param_copy(i, s, s).wait_recv()
    prm_ref[...] = jnp.zeros_like(prm_ref)
    wide = got[3].shape[2]
    for q in range(sp):
        for kind in range(2):
            for d in range(2):
                at = slice(d * heads + q * wide, d * heads + (q + 1) * wide)
                prm_ref[kind : kind + 1, at] = got[3 + kind][q, d : d + 1, :]
        off = 0
        for i in range(3):
            n = got[i].shape[2]
            w_ref[0:4, off + q * n : off + (q + 1) * n] = got[i][q].astype(F32)
            off += n * sp
    rate = jax.nn.softplus(inc + prm_ref[0:1, :])
    log_decay = -jnp.exp(prm_ref[1:2, :]) * rate + spikes
    lower = (lane <= row).astype(F32)
    upper = (lane >= row).astype(F32)
    cum_f = jnp.dot(lower, log_decay, precision=HIGHEST, preferred_element_type=F32)
    cum_b = jnp.dot(upper, log_decay, precision=HIGHEST, preferred_element_type=F32)
    cum = jnp.where(lane < heads, cum_f, cum_b)
    lane1 = lane[0:1]
    last = jnp.where(lane1 < heads, cum_f[blk - 1 : blk], cum_b[0:1])
    cum_ref[...] = cum
    rate_ref[...] = rate
    cum_t[...] = cum.T
    rate_t[...] = rate.T
    fac_ref[...] = rate * jnp.exp(last - cum)
    first_log[...] = jnp.broadcast_to(last, (8, 128))

    def rolled(ref, p):
        return pltpu.roll(ref[...], lax.rem(128 - p * per_pair, 128), 1)

    def two(cols, i):
        return jnp.where(left, cols[:, i : i + 1], cols[:, i + 1 : i + 2])

    def conv(src, col, width, off):
        at = pl.ds(pl.multiple_of(off + col, 128), width)
        v = src[:, pl.ds(pl.multiple_of(col, 128), width)].astype(F32)
        r = lax.broadcasted_iota(jnp.int32, (blk, width), 0)
        h0, h1, h2 = halo_ref[0:1, at], halo_ref[1:2, at], halo_ref[2:3, at]
        m1 = jnp.where(r == 0, h1, pltpu.roll(v, 1, 0))
        m2 = jnp.where(r == 0, h0, jnp.where(r == 1, h1, pltpu.roll(v, 2, 0)))
        p1 = jnp.where(r == blk - 1, h2, pltpu.roll(v, blk - 1, 0))
        s = m2 * w_ref[0:1, at] + m1 * w_ref[1:2, at] + v * w_ref[2:3, at] + p1 * w_ref[3:4, at]
        return (s / (1.0 + jnp.exp(-s))).astype(BF16)

    x_total = x_ref.shape[1]
    b_total = b_ref.shape[1]

    def first(p, _):
        x_at = pl.ds(pl.multiple_of(p * x_w, 128), x_w)
        b_at = pl.ds(pl.multiple_of(p * b_w, 128), b_w)
        xv = conv(x_ref, p * x_w, x_w, 0)
        bv = conv(b_ref, p * b_w, b_w, x_total)
        xc[:, x_at] = xv
        bc[:, b_at] = bv
        cc[:, b_at] = conv(c_ref, p * b_w, b_w, x_total + b_total)
        cols = rolled(fac_ref, p)
        xf = xv.astype(F32)
        for d in range(2):
            scaled = jnp.concatenate(
                [
                    (xf[:, k * 128 : (k + 1) * 128] * two(cols, d * heads + 2 * k)).astype(BF16)
                    for k in range(tiles)
                ],
                axis=1,
            )
            u = lax.dot_general(scaled, bv, (((0,), (0,)), ((), ())), preferred_element_type=F32)
            half = x_w // 2
            rows = pl.ds(pl.multiple_of(p * x_w, 128), x_w)
            first_total[d, rows, :] = jnp.concatenate(
                [u[:half, :STATE], u[half:, STATE:]], axis=0
            ).astype(BF16)
        return 0

    for direction, present in ((0, has_prev), (1, has_next)):

        @pl.when(present)
        def _(direction=direction):
            for i in range(3):
                edge_copy(i, direction).wait_recv()

    off = 0
    for i in range(3):
        n = edges[i].shape[1]
        low = edges[i][...].astype(F32)
        high = edges[3 + i][...].astype(F32)
        halo_ref[0:2, off : off + n] = jnp.where(has_prev, low[EDGE - 2 :], 0.0)
        halo_ref[2:3, off : off + n] = jnp.where(has_next, high[0:1], 0.0)
        off += n
    lax.fori_loop(0, pairs, first, 0)
    for o in range(1, sp):
        for i in range(5):
            param_copy(i, lax.rem(here + o, sp), here).wait_send()
    for direction, present in ((0, has_next), (1, has_prev)):

        @pl.when(present)
        def _(direction=direction):
            for i in range(3):
                edge_copy(i, direction).wait_send()


    def inner(p, _):
        x_at = pl.ds(pl.multiple_of(p * x_w, 128), x_w)
        b_at = pl.ds(pl.multiple_of(p * b_w, 128), b_w)
        bv, cv, xv = bc[:, b_at], cc[:, b_at], xc[:, x_at]
        cols = rolled(cum_ref, p)
        parts = []
        for g in range(2):
            scores = lax.dot_general(
                cv[:, g * STATE : (g + 1) * STATE],
                bv[:, g * STATE : (g + 1) * STATE],
                (((1,), (1,)), ((), ())),
                preferred_element_type=F32,
            )
            for i in range(per_pair // 2):
                h = g * (per_pair // 2) + i
                hf = p * per_pair + h
                gap_f = cols[:, h : h + 1] - cum_t[pl.ds(hf, 1), :]
                gap_b = cols[:, heads + h : heads + h + 1] - cum_t[pl.ds(heads + hf, 1), :]
                gap = jnp.where(lane < row, gap_f, jnp.where(lane > row, gap_b, 0.0))
                rf, rb = rate_t[pl.ds(hf, 1), :], rate_t[pl.ds(heads + hf, 1), :]
                scale = jnp.where(lane < row, rf, jnp.where(lane > row, rb, rf + rb))
                parts.append((scores * jnp.exp(gap) * scale).astype(BF16))
        for k in range(tiles):
            xt = xv[:, k * 128 : (k + 1) * 128]
            zero = jnp.zeros_like(xt)
            both = jnp.concatenate([jnp.where(left, xt, zero), jnp.where(left, zero, xt)], axis=0)
            w = jnp.concatenate([parts[2 * k], parts[2 * k + 1]], axis=1)
            y_ref[:, pl.ds(pl.multiple_of(p * x_w + k * 128, 128), 128)] = jnp.dot(
                w, both, preferred_element_type=F32
            )
        return 0

    def copy(src, dst, send, recv, level, member):
        return pltpu.make_async_remote_copy(
            src_ref=src,
            dst_ref=dst,
            send_sem=send,
            recv_sem=recv,
            device_id=member_id(level, member),
            device_id_type=pl.DeviceIdType.MESH,
        )

    def expand(slot, tile):
        decay[slot] = jnp.exp(jnp.broadcast_to(tile[0:1, :], (128, 128)).T)

    slots = len(levels) + 1
    cuts = [(i * pairs) // slots for i in range(slots + 1)]
    base = jnp.int32(0)
    bases = []
    for k, level in enumerate(levels):
        n = level[1]
        me = digit_of(level)
        total, log = totals[k], logs[k]
        rows = total.shape[1] // n
        sem = sems[k]
        pending = []
        for o in range(1, n):
            m = lax.rem(me + o, n)
            part = total.at[:, pl.ds(pl.multiple_of(m * rows, 64), rows), :]
            pending.append(copy(part, up[k].at[me], sem.at[0, m], sem.at[1, me], level, m))
            pending.append(copy(log, up_log[k].at[me], sem.at[2, m], sem.at[3, me], level, m))
        for one in pending:
            one.start()
        up[k][me] = total[:, pl.ds(pl.multiple_of(me * rows, 64), rows), :]
        up_log[k][me] = log[...]
        lax.fori_loop(cuts[k], cuts[k + 1], inner, 0)
        for one in pending:
            one.wait_send()
        for o in range(1, n):
            s = lax.rem(me + o, n)
            part = total.at[:, pl.ds(0, rows), :]
            copy(part, up[k].at[s], sem.at[0, s], sem.at[1, s], level, s).wait_recv()
            copy(log, up_log[k].at[s], sem.at[2, s], sem.at[3, s], level, s).wait_recv()
        base = base + me * (rows // HEAD_DIM)
        bases.append(base)
        log_sum = up_log[k][0]
        for m in range(1, n):
            log_sum = log_sum + up_log[k][m]
        logs[k + 1][...] = log_sum
        for m in range(n):
            expand(m, up_log[k][m])

        def gather(h, _, k=k, n=n, base=base):
            at = pl.ds(pl.multiple_of(h * HEAD_DIM, HEAD_DIM), HEAD_DIM)
            f = up[k][0, 0, at, :].astype(F32)
            b = up[k][n - 1, 1, at, :].astype(F32)
            for m in range(1, n):
                f = f * decay[m, pl.ds(base + h, 1), :] + up[k][m, 0, at, :].astype(F32)
                r = n - 1 - m
                b = b * decay[r, pl.ds(heads + base + h, 1), :] + up[k][r, 1, at, :].astype(F32)
            totals[k + 1][0, at, :] = f.astype(BF16)
            totals[k + 1][1, at, :] = b.astype(BF16)
            return 0

        lax.fori_loop(0, rows // HEAD_DIM, gather, 0)

    n = top[1]
    me = digit_of(top)
    total, log = totals[-1], logs[-1]
    pending = []
    for o in range(1, n):
        m = lax.rem(me + o, n)
        d = jnp.where(m < me, 1, 0)
        pending.append(
            copy(total.at[d], top_in.at[me], top_sem.at[0, m], top_sem.at[1, me], top, m)
        )
        pending.append(copy(log, top_log.at[me], top_sem.at[2, m], top_sem.at[3, me], top, m))
    for one in pending:
        one.start()
    lax.fori_loop(cuts[-2], cuts[-1], inner, 0)
    for one in pending:
        one.wait_send()
    for o in range(1, n):
        s = lax.rem(me + o, n)
        copy(total.at[0], top_in.at[s], top_sem.at[0, s], top_sem.at[1, s], top, s).wait_recv()
        copy(log, top_log.at[s], top_sem.at[2, s], top_sem.at[3, s], top, s).wait_recv()
    incoming[...] = jnp.zeros_like(incoming)

    def carry(s, d):
        expand(0, top_log[s])

        def one_head(h, _):
            at = pl.ds(pl.multiple_of(h * HEAD_DIM, HEAD_DIM), HEAD_DIM)
            factor = decay[0, pl.ds(d * heads + base + h, 1), :]
            incoming[d, at, :] = incoming[d, at, :] * factor + top_in[s, at, :].astype(F32)
            return 0

        lax.fori_loop(0, total.shape[1] // HEAD_DIM, one_head, 0)
        return 0

    lax.fori_loop(0, me, lambda s, _: carry(s, 0), 0)
    lax.fori_loop(0, n - 1 - me, lambda i, _: carry(n - 1 - i, 1), 0)

    for k in reversed(range(len(levels))):
        level = levels[k]
        n = level[1]
        me = digit_of(level)
        sem = sems[k]
        rows = totals[k].shape[1] // n
        source = incoming if k == len(levels) - 1 else down[k + 1]
        for m in range(n):
            expand(m, up_log[k][m])

        def spread(h, _, k=k, n=n, base=bases[k], source=source):
            at = pl.ds(pl.multiple_of(h * HEAD_DIM, HEAD_DIM), HEAD_DIM)
            f = source[0, at, :].astype(F32)
            b = source[1, at, :].astype(F32)
            for m in range(n):
                r = n - 1 - m
                stage[k][m, 0, at, :] = f.astype(BF16)
                stage[k][r, 1, at, :] = b.astype(BF16)
                if m < n - 1:
                    f = f * decay[m, pl.ds(base + h, 1), :] + up[k][m, 0, at, :].astype(F32)
                    b = b * decay[r, pl.ds(heads + base + h, 1), :] + up[k][r, 1, at, :].astype(F32)
            return 0

        lax.fori_loop(0, rows // HEAD_DIM, spread, 0)
        mine = pl.ds(pl.multiple_of(me * rows, 64), rows)
        pending = []
        for o in range(1, n):
            m = lax.rem(me + o, n)
            pending.append(
                copy(stage[k].at[m], down[k].at[:, mine, :], sem.at[4, m], sem.at[5, me], level, m)
            )
        for one in pending:
            one.start()
        down[k][:, mine, :] = stage[k][me]
        for one in pending:
            one.wait_send()
        for o in range(1, n):
            s = lax.rem(me + o, n)
            theirs = pl.ds(pl.multiple_of(s * rows, 64), rows)
            copy(
                stage[k].at[s], down[k].at[:, theirs, :], sem.at[4, s], sem.at[5, s], level, s
            ).wait_recv()

    final = down[0] if levels else incoming
    cum_ref[...] = jnp.exp(cum_ref[...])

    def last_part(p, _):
        x_at = pl.ds(pl.multiple_of(p * x_w, 128), x_w)
        cv = cc[:, pl.ds(pl.multiple_of(p * b_w, 128), b_w)]
        cols = rolled(cum_ref, p)
        carried = []
        for d in range(2):
            st = final[d, x_at, :].astype(BF16)
            got = [
                lax.dot_general(
                    cv[:, g * STATE : (g + 1) * STATE],
                    st,
                    (((1,), (1,)), ((), ())),
                    preferred_element_type=F32,
                )
                for g in range(2)
            ]
            carried.append(got)
        for k in range(tiles):
            cut = slice(k * 128, (k + 1) * 128)
            at = pl.ds(pl.multiple_of(p * x_w + k * 128, 128), 128)
            y = y_ref[:, at]
            for d in range(2):
                a, b = carried[d][0][:, cut], carried[d][1][:, cut]
                if 2 * k + 1 < per_pair // 2:
                    v = a
                elif 2 * k >= per_pair // 2:
                    v = b
                else:
                    v = jnp.where(left, a, b)
                y = y + v * two(cols, d * heads + 2 * k)
            z = z_ref[:, at].astype(F32)
            gated = y.astype(BF16).astype(F32) * (z / (1.0 + jnp.exp(-z)))
            square = gated * gated
            low = jnp.sum(jnp.where(left, square, 0.0), axis=1, keepdims=True)
            high = jnp.sum(jnp.where(left, 0.0, square), axis=1, keepdims=True)
            mean = jnp.where(left, low, high) * (1.0 / HEAD_DIM)
            out_ref[:, at] = (gated * lax.rsqrt(mean + 1e-6) * gain_ref[0:1, at]).astype(BF16)
        return 0

    lax.fori_loop(0, pairs, last_part, 0)


def local(sp, dp, x, b, c, z, ahead, back, spike, wx, wb, wc, offset, fading, gain):
    x, b, c, z = x[0], b[0], c[0], z[0]
    blk, x_total = x.shape
    groups = b.shape[1] // STATE
    heads = ahead.shape[2]
    pairs = groups // 2
    levels, top = levels_of(sp, dp, groups)
    scratch = [
        pltpu.VMEM((blk, x_total), BF16),
        pltpu.VMEM((blk, groups * STATE), BF16),
        pltpu.VMEM((blk, groups * STATE), BF16),
        pltpu.VMEM((blk, x_total), F32),
    ]
    scratch += [pltpu.VMEM((128, 128), F32)] * 5
    rows = x_total
    params = (wx, wb, wc, offset, fading)
    width = x_total + 2 * b.shape[1]
    early = [pltpu.VMEM((sp,) + one.shape, one.dtype) for one in params]
    early += [pltpu.VMEM((8, width), F32), pltpu.VMEM((8, 128), F32), pltpu.VMEM((8, width), F32)]
    early += [pltpu.VMEM((EDGE, one.shape[1]), BF16) for one in (x, b, c)] * 2
    early += [pltpu.SemaphoreType.DMA((2, 5, sp)), pltpu.SemaphoreType.DMA((2, 2, 3))]
    scratch += [pltpu.VMEM((2, rows, STATE), BF16), pltpu.VMEM((8, 128), F32)]
    scratch += early
    widest = 1
    for _, n, _ in levels:
        widest = max(widest, n)
        scratch += [
            pltpu.VMEM((n, 2, rows // n, STATE), BF16),
            pltpu.VMEM((n, 8, 128), F32),
            pltpu.VMEM((2, rows, STATE), BF16),
            pltpu.VMEM((n, 2, rows // n, STATE), BF16),
            pltpu.VMEM((2, rows // n, STATE), BF16),
            pltpu.VMEM((8, 128), F32),
            pltpu.SemaphoreType.DMA((6, n)),
        ]
        rows //= n
    scratch += [
        pltpu.VMEM((top[1], rows, STATE), BF16),
        pltpu.VMEM((top[1], 8, 128), F32),
        pltpu.SemaphoreType.DMA((4, top[1])),
        pltpu.VMEM((2, rows, STATE), F32),
        pltpu.VMEM((widest, 128, 128), F32),
    ]
    out = pl.pallas_call(
        functools.partial(kernel, levels, top, (heads, pairs, sp, dp)),
        out_shape=jax.ShapeDtypeStruct((blk, x_total), BF16),
        in_specs=[pl.BlockSpec(memory_space=pltpu.VMEM)] * 13,
        out_specs=pl.BlockSpec(memory_space=pltpu.VMEM),
        scratch_shapes=scratch,
        compiler_params=pltpu.CompilerParams(
            collective_id=0, has_side_effects=True, vmem_limit_bytes=60 * 2**20
        ),
        name="mixer",
    )(x, b, c, z, ahead[0].T, back[0].T, spike[0].T, *params, gain.astype(F32)[None])
    return out[None]


def solution(mesh):
    tokens = P("dp", "sp", None)
    placed = (tokens,) * 7 + (P(None, "sp"),) * 5 + (P(),)
    return jax.shard_map(
        functools.partial(local, mesh.shape["sp"], mesh.shape["dp"]),
        mesh=mesh,
        in_specs=placed,
        out_specs=tokens,
        check_vma=False,
    )
```

```python
import functools

import jax
import jax.numpy as jnp
from jax import lax
from jax.experimental import pallas as pl
from jax.experimental.pallas import tpu as pltpu
from jax.sharding import PartitionSpec as P

F32 = jnp.float32
BF16 = jnp.bfloat16
HEAD_DIM = 64
STATE = 128
EDGE = 8
HIGHEST = lax.Precision.HIGHEST


def levels_of(sp, dp, groups):
    found = []
    split = 1
    core = 2 if sp % 2 == 0 else 1
    inner = 2 if dp % 2 == 0 and groups % (2 * sp) == 0 else 1
    for axis, count, stride in (("sp", core, 1), ("sp", sp // core, core), ("dp", inner, 1)):
        if count > 1:
            found.append((axis, count, stride))
            split *= count
    return tuple(found), ("dp", dp // inner, inner)


def digit_of(level):
    axis, count, stride = level
    return lax.rem(lax.axis_index(axis) // stride, count)


def member_id(level, member):
    axis, count, stride = level
    return {axis: lax.axis_index(axis) + (member - digit_of(level)) * stride}


def kernel(levels, top, sizes, *refs):
    heads, pairs, chunks, sp, dp = sizes
    (x_ref, b_ref, c_ref, z_ref, ahead_ref, back_ref, spike_ref) = refs[:7]
    params = refs[7:12]
    gain_ref, out_ref = refs[12:14]
    (xc, bc, cc, y_ref, cum_ref, rate_ref, cum_t, rate_t, fac_ref) = refs[14:23]
    refs = refs[:14] + refs[23:]
    got, w_ref, prm_ref, halo_ref, edges, early_sem, edge_sem = (
        refs[14:19], refs[19], refs[20], refs[21], refs[22:28], refs[28], refs[29]
    )
    rest = list(refs[30:])
    depth = len(levels)
    logs = [rest.pop(0) for _ in range(depth + 1)]
    up_log = [rest.pop(0) for _ in range(depth + 1)]
    decay = [rest.pop(0) for _ in range(depth + 1)]
    log_sem = [rest.pop(0) for _ in range(depth + 1)]
    totals, up, down, stage, sems, incoming = ([] for _ in range(6))
    for _ in range(chunks):
        totals.append([rest.pop(0) for _ in range(depth + 1)])
        up.append([rest.pop(0) for _ in range(depth + 1)])
        down.append([rest.pop(0) for _ in range(depth)])
        stage.append([rest.pop(0) for _ in range(depth)])
        sems.append([rest.pop(0) for _ in range(depth + 1)])
        incoming.append(rest.pop(0))
    blk = x_ref.shape[0]
    per_pair = heads // pairs
    x_w = per_pair * HEAD_DIM
    b_w = 2 * STATE
    tiles = x_w // 128
    lane = lax.broadcasted_iota(jnp.int32, (blk, 128), 1)
    left = lane < HEAD_DIM
    row = lax.broadcasted_iota(jnp.int32, (blk, 128), 0)

    segment = ("sp", sp, 1)
    here, there = lax.axis_index("sp"), lax.axis_index("dp")
    rank = there * sp + here
    has_next, has_prev = rank < sp * dp - 1, rank > 0
    after = {"sp": lax.rem(here + 1, sp), "dp": lax.rem(there + (here + 1) // sp, dp)}
    before = {
        "sp": lax.rem(here + sp - 1, sp),
        "dp": lax.rem(there + dp - (sp - here) // sp, dp),
    }
    mesh_id = pl.DeviceIdType.MESH
    barrier = pltpu.get_barrier_semaphore()
    greeted = 0
    for level in levels + (top, segment):
        me = digit_of(level)
        for o in range(1, level[1]):
            target = member_id(level, lax.rem(me + o, level[1]))
            pl.semaphore_signal(barrier, inc=1, device_id=target, device_id_type=mesh_id)
            greeted += 1
    for present, target in ((has_next, after), (has_prev, before)):

        @pl.when(present)
        def _(target=target):
            pl.semaphore_signal(barrier, inc=1, device_id=target, device_id_type=mesh_id)

    filler = jnp.zeros((128 - 2 * heads, blk), F32)
    inc = jnp.concatenate([ahead_ref[...], back_ref[...], filler], axis=0).T
    spikes = jnp.concatenate([spike_ref[...], spike_ref[...], filler], axis=0).T
    count = sp * dp
    neighbours = (rank + count - 1) // count + (2 * count - 2 - rank) // count
    pl.semaphore_wait(barrier, greeted + neighbours)

    def edge_copy(i, direction):
        src = (x_ref, b_ref, c_ref)[i]
        start = blk - EDGE if direction == 0 else 0
        return pltpu.make_async_remote_copy(
            src_ref=src.at[pl.ds(start, EDGE), :],
            dst_ref=edges[3 * direction + i],
            send_sem=edge_sem.at[0, direction, i],
            recv_sem=edge_sem.at[1, direction, i],
            device_id=(after, before)[direction],
            device_id_type=mesh_id,
        )

    def param_copy(i, member, slot):
        return pltpu.make_async_remote_copy(
            src_ref=params[i],
            dst_ref=got[i].at[slot],
            send_sem=early_sem.at[0, i, member],
            recv_sem=early_sem.at[1, i, slot],
            device_id=member_id(segment, member),
            device_id_type=mesh_id,
        )

    for o in range(1, sp):
        for i in range(5):
            param_copy(i, lax.rem(here + o, sp), here).start()
    for direction, present in ((0, has_next), (1, has_prev)):

        @pl.when(present)
        def _(direction=direction):
            for i in range(3):
                edge_copy(i, direction).start()

    for i in range(5):
        got[i][here] = params[i][...]
    for o in range(1, sp):
        for i in range(5):
            s = lax.rem(here + o, sp)
            param_copy(i, s, s).wait_recv()
    prm_ref[...] = jnp.zeros_like(prm_ref)
    wide = got[3].shape[2]
    for q in range(sp):
        for kind in range(2):
            for d in range(2):
                at = slice(d * heads + q * wide, d * heads + (q + 1) * wide)
                prm_ref[kind : kind + 1, at] = got[3 + kind][q, d : d + 1, :]
        off = 0
        for i in range(3):
            n = got[i].shape[2]
            w_ref[0:4, off + q * n : off + (q + 1) * n] = got[i][q].astype(F32)
            off += n * sp
    rate = jax.nn.softplus(inc + prm_ref[0:1, :])
    log_decay = -jnp.exp(prm_ref[1:2, :]) * rate + spikes
    lower = (lane <= row).astype(F32)
    upper = (lane >= row).astype(F32)
    cum_f = jnp.dot(lower, log_decay, precision=HIGHEST, preferred_element_type=F32)
    cum_b = jnp.dot(upper, log_decay, precision=HIGHEST, preferred_element_type=F32)
    cum = jnp.where(lane < heads, cum_f, cum_b)
    lane1 = lane[0:1]
    last = jnp.where(lane1 < heads, cum_f[blk - 1 : blk], cum_b[0:1])
    cum_ref[...] = cum
    rate_ref[...] = rate
    cum_t[...] = cum.T
    rate_t[...] = rate.T
    fac_ref[...] = rate * jnp.exp(last - cum)
    logs[0][...] = jnp.broadcast_to(last, (8, 128))

    def rolled(ref, p):
        return pltpu.roll(ref[...], lax.rem(128 - p * per_pair, 128), 1)

    def two(cols, i):
        return jnp.where(left, cols[:, i : i + 1], cols[:, i + 1 : i + 2])

    def conv(src, col, width, off):
        at = pl.ds(pl.multiple_of(off + col, 128), width)
        v = src[:, pl.ds(pl.multiple_of(col, 128), width)].astype(F32)
        r = lax.broadcasted_iota(jnp.int32, (blk, width), 0)
        h0, h1, h2 = halo_ref[0:1, at], halo_ref[1:2, at], halo_ref[2:3, at]
        m1 = jnp.where(r == 0, h1, pltpu.roll(v, 1, 0))
        m2 = jnp.where(r == 0, h0, jnp.where(r == 1, h1, pltpu.roll(v, 2, 0)))
        p1 = jnp.where(r == blk - 1, h2, pltpu.roll(v, blk - 1, 0))
        s = m2 * w_ref[0:1, at] + m1 * w_ref[1:2, at] + v * w_ref[2:3, at] + p1 * w_ref[3:4, at]
        return (s / (1.0 + jnp.exp(-s))).astype(BF16)

    share = pairs // chunks
    x_total = x_ref.shape[1]
    b_total = b_ref.shape[1]

    def first(c, p, _):
        x_at = pl.ds(pl.multiple_of(p * x_w, 128), x_w)
        b_at = pl.ds(pl.multiple_of(p * b_w, 128), b_w)
        xv = conv(x_ref, p * x_w, x_w, 0)
        bv = conv(b_ref, p * b_w, b_w, x_total)
        xc[:, x_at] = xv
        bc[:, b_at] = bv
        cc[:, b_at] = conv(c_ref, p * b_w, b_w, x_total + b_total)
        cols = rolled(fac_ref, p)
        xf = xv.astype(F32)
        for d in range(2):
            scaled = jnp.concatenate(
                [
                    (xf[:, k * 128 : (k + 1) * 128] * two(cols, d * heads + 2 * k)).astype(BF16)
                    for k in range(tiles)
                ],
                axis=1,
            )
            u = lax.dot_general(scaled, bv, (((0,), (0,)), ((), ())), preferred_element_type=F32)
            half = x_w // 2
            rows = pl.ds(pl.multiple_of((p - c * share) * x_w, 128), x_w)
            totals[c][0][d, rows, :] = jnp.concatenate(
                [u[:half, :STATE], u[half:, STATE:]], axis=0
            ).astype(BF16)
        return 0

    for direction, present in ((0, has_prev), (1, has_next)):

        @pl.when(present)
        def _(direction=direction):
            for i in range(3):
                edge_copy(i, direction).wait_recv()

    off = 0
    for i in range(3):
        n = edges[i].shape[1]
        low = edges[i][...].astype(F32)
        high = edges[3 + i][...].astype(F32)
        halo_ref[0:2, off : off + n] = jnp.where(has_prev, low[EDGE - 2 :], 0.0)
        halo_ref[2:3, off : off + n] = jnp.where(has_next, high[0:1], 0.0)
        off += n
    def inner(p, _):
        x_at = pl.ds(pl.multiple_of(p * x_w, 128), x_w)
        b_at = pl.ds(pl.multiple_of(p * b_w, 128), b_w)
        bv, cv, xv = bc[:, b_at], cc[:, b_at], xc[:, x_at]
        cols = rolled(cum_ref, p)
        parts = []
        for g in range(2):
            scores = lax.dot_general(
                cv[:, g * STATE : (g + 1) * STATE],
                bv[:, g * STATE : (g + 1) * STATE],
                (((1,), (1,)), ((), ())),
                preferred_element_type=F32,
            )
            for i in range(per_pair // 2):
                h = g * (per_pair // 2) + i
                hf = p * per_pair + h
                gap_f = cols[:, h : h + 1] - cum_t[pl.ds(hf, 1), :]
                gap_b = cols[:, heads + h : heads + h + 1] - cum_t[pl.ds(heads + hf, 1), :]
                gap = jnp.where(lane < row, gap_f, jnp.where(lane > row, gap_b, 0.0))
                rf, rb = rate_t[pl.ds(hf, 1), :], rate_t[pl.ds(heads + hf, 1), :]
                scale = jnp.where(lane < row, rf, jnp.where(lane > row, rb, rf + rb))
                parts.append((scores * jnp.exp(gap) * scale).astype(BF16))
        for k in range(tiles):
            xt = xv[:, k * 128 : (k + 1) * 128]
            zero = jnp.zeros_like(xt)
            both = jnp.concatenate([jnp.where(left, xt, zero), jnp.where(left, zero, xt)], axis=0)
            w = jnp.concatenate([parts[2 * k], parts[2 * k + 1]], axis=1)
            y_ref[:, pl.ds(pl.multiple_of(p * x_w + k * 128, 128), 128)] = jnp.dot(
                w, both, preferred_element_type=F32
            )
        return 0

    def copy(src, dst, send, recv, level, member):
        return pltpu.make_async_remote_copy(
            src_ref=src,
            dst_ref=dst,
            send_sem=send,
            recv_sem=recv,
            device_id=member_id(level, member),
            device_id_type=pl.DeviceIdType.MESH,
        )

    every_level = levels + (top,)
    head_share = heads // chunks
    bases = [jnp.int32(0)]
    size = head_share
    for level in levels:
        size = size // level[1]
        bases.append(bases[-1] + digit_of(level) * size)
    pending = [[] for _ in range(chunks)]

    def head_rows(h):
        return pl.ds(pl.multiple_of(h * HEAD_DIM, HEAD_DIM), HEAD_DIM)

    def log_copy(k, member, slot):
        sem = log_sem[k]
        return copy(
            logs[k], up_log[k].at[slot], sem.at[0, member], sem.at[1, slot], every_level[k], member
        )

    def start_up(c, k):
        level = every_level[k]
        n, me = level[1], digit_of(level)
        total, sem = totals[c][k], sems[c][k]
        rows = total.shape[1] // n
        for o in range(1, n):
            m = lax.rem(me + o, n)
            if c == 0:
                pending[c].append(log_copy(k, m, me))
            if k < depth:
                part = total.at[:, pl.ds(pl.multiple_of(m * rows, 64), rows), :]
            else:
                part = total.at[jnp.where(m < me, 1, 0)]
            pending[c].append(
                copy(part, up[c][k].at[me], sem.at[0, m], sem.at[1, me], level, m)
            )
        for one in pending[c]:
            one.start()
        if k < depth:
            up[c][k][me] = total[:, pl.ds(pl.multiple_of(me * rows, 64), rows), :]
        if c == 0:
            up_log[k][me] = logs[k][...]

    def flush(c):
        for one in pending[c]:
            one.wait_send()
        pending[c].clear()

    def finish_up(c, k):
        level = every_level[k]
        n, me = level[1], digit_of(level)
        total, sem = totals[c][k], sems[c][k]
        flush(c)
        for o in range(1, n):
            s = lax.rem(me + o, n)
            if c == 0:
                log_copy(k, s, s).wait_recv()
            part = total.at[:, pl.ds(0, total.shape[1] // n), :] if k < depth else total.at[0]
            copy(part, up[c][k].at[s], sem.at[0, s], sem.at[1, s], level, s).wait_recv()
        if c == 0:

            def expand(m, _):
                decay[k][m] = jnp.exp(jnp.broadcast_to(up_log[k][m][0:1, :], (128, 128)).T)
                return 0

            lax.fori_loop(0, n, expand, 0)
            if k < depth:
                log_sum = up_log[k][0]
                for m in range(1, n):
                    log_sum = log_sum + up_log[k][m]
                logs[k + 1][...] = log_sum

    def gather(c, k):
        n = levels[k][1]
        base = c * head_share + bases[k + 1]
        part, new = up[c][k], totals[c][k + 1]

        def one_head(h, _):
            at = head_rows(h)
            f = part[0, 0, at, :].astype(F32)
            b = part[n - 1, 1, at, :].astype(F32)
            for m in range(1, n):
                r = n - 1 - m
                f = f * decay[k][m, pl.ds(base + h, 1), :] + part[m, 0, at, :].astype(F32)
                b = b * decay[k][r, pl.ds(heads + base + h, 1), :] + part[r, 1, at, :].astype(F32)
            new[0, at, :] = f.astype(BF16)
            new[1, at, :] = b.astype(BF16)
            return 0

        lax.fori_loop(0, new.shape[1] // HEAD_DIM, one_head, 0)

    def enter(c):
        n, me = top[1], digit_of(top)
        base = c * head_share + bases[-1]
        into = incoming[c]
        into[...] = jnp.zeros_like(into)

        def carry(s, d):
            def one_head(h, _):
                at = head_rows(h)
                factor = decay[depth][s, pl.ds(d * heads + base + h, 1), :]
                into[d, at, :] = into[d, at, :] * factor + up[c][depth][s, at, :].astype(F32)
                return 0

            lax.fori_loop(0, into.shape[1] // HEAD_DIM, one_head, 0)
            return 0

        lax.fori_loop(0, me, lambda s, _: carry(s, 0), 0)
        lax.fori_loop(0, n - 1 - me, lambda i, _: carry(n - 1 - i, 1), 0)

    def start_down(c, k):
        level = levels[k]
        n, me = level[1], digit_of(level)
        sem = sems[c][k]
        rows = totals[c][k].shape[1] // n
        base = c * head_share + bases[k + 1]
        source = incoming[c] if k == depth - 1 else down[c][k + 1]
        part, out = up[c][k], stage[c][k]

        def spread(h, _):
            at = head_rows(h)
            f = source[0, at, :].astype(F32)
            b = source[1, at, :].astype(F32)
            for m in range(n):
                r = n - 1 - m
                out[m, 0, at, :] = f.astype(BF16)
                out[r, 1, at, :] = b.astype(BF16)
                if m < n - 1:
                    f = f * decay[k][m, pl.ds(base + h, 1), :] + part[m, 0, at, :].astype(F32)
                    down_factor = decay[k][r, pl.ds(heads + base + h, 1), :]
                    b = b * down_factor + part[r, 1, at, :].astype(F32)
            return 0

        lax.fori_loop(0, rows // HEAD_DIM, spread, 0)
        mine = pl.ds(pl.multiple_of(me * rows, 64), rows)
        for o in range(1, n):
            m = lax.rem(me + o, n)
            pending[c].append(
                copy(out.at[m], down[c][k].at[:, mine, :], sem.at[2, m], sem.at[3, me], level, m)
            )
        for one in pending[c]:
            one.start()
        down[c][k][:, mine, :] = out[me]

    def finish_down(c, k):
        level = levels[k]
        n, me = level[1], digit_of(level)
        sem = sems[c][k]
        rows = totals[c][k].shape[1] // n
        flush(c)
        for o in range(1, n):
            s = lax.rem(me + o, n)
            theirs = pl.ds(pl.multiple_of(s * rows, 64), rows)
            copy(
                stage[c][k].at[s], down[c][k].at[:, theirs, :], sem.at[2, s], sem.at[3, s], level, s
            ).wait_recv()

    for c in range(chunks):
        lax.fori_loop(c * share, (c + 1) * share, functools.partial(first, c), 0)
        start_up(c, 0)
    for o in range(1, sp):
        for i in range(5):
            param_copy(i, lax.rem(here + o, sp), here).wait_send()
    for direction, present in ((0, has_next), (1, has_prev)):

        @pl.when(present)
        def _(direction=direction):
            for i in range(3):
                edge_copy(i, direction).wait_send()


    gaps = chunks * depth
    cuts = [(i * pairs) // gaps for i in range(gaps + 1)]
    for k in range(depth):
        for c in range(chunks):
            finish_up(c, k)
            gather(c, k)
            start_up(c, k + 1)
            at = k * chunks + c
            lax.fori_loop(cuts[at], cuts[at + 1], inner, 0)
    for c in range(chunks):
        finish_up(c, depth)
        enter(c)
        start_down(c, depth - 1)
    for k in reversed(range(1, depth)):
        for c in range(chunks):
            finish_down(c, k)
            start_down(c, k - 1)

    cum_ref[...] = jnp.exp(cum_ref[...])

    def last_part(c, p, _):
        cv = cc[:, pl.ds(pl.multiple_of(p * b_w, 128), b_w)]
        cols = rolled(cum_ref, p)
        carried = []
        for d in range(2):
            st = down[c][0][d, pl.ds(pl.multiple_of((p - c * share) * x_w, 128), x_w), :]
            got = [
                lax.dot_general(
                    cv[:, g * STATE : (g + 1) * STATE],
                    st,
                    (((1,), (1,)), ((), ())),
                    preferred_element_type=F32,
                )
                for g in range(2)
            ]
            carried.append(got)
        for k in range(tiles):
            cut = slice(k * 128, (k + 1) * 128)
            at = pl.ds(pl.multiple_of(p * x_w + k * 128, 128), 128)
            y = y_ref[:, at]
            for d in range(2):
                a, b = carried[d][0][:, cut], carried[d][1][:, cut]
                if 2 * k + 1 < per_pair // 2:
                    v = a
                elif 2 * k >= per_pair // 2:
                    v = b
                else:
                    v = jnp.where(left, a, b)
                y = y + v * two(cols, d * heads + 2 * k)
            z = z_ref[:, at].astype(F32)
            gated = y.astype(BF16).astype(F32) * (z / (1.0 + jnp.exp(-z)))
            square = gated * gated
            low = jnp.sum(jnp.where(left, square, 0.0), axis=1, keepdims=True)
            high = jnp.sum(jnp.where(left, 0.0, square), axis=1, keepdims=True)
            mean = jnp.where(left, low, high) * (1.0 / HEAD_DIM)
            out_ref[:, at] = (gated * lax.rsqrt(mean + 1e-6) * gain_ref[0:1, at]).astype(BF16)
        return 0

    for c in range(chunks):
        finish_down(c, 0)
        lax.fori_loop(c * share, (c + 1) * share, functools.partial(last_part, c), 0)


def local(sp, dp, x, b, c, z, ahead, back, spike, wx, wb, wc, offset, fading, gain):
    x, b, c, z = x[0], b[0], c[0], z[0]
    blk, x_total = x.shape
    groups = b.shape[1] // STATE
    heads = ahead.shape[2]
    pairs = groups // 2
    levels, top = levels_of(sp, dp, groups)
    scratch = [
        pltpu.VMEM((blk, x_total), BF16),
        pltpu.VMEM((blk, groups * STATE), BF16),
        pltpu.VMEM((blk, groups * STATE), BF16),
        pltpu.VMEM((blk, x_total), F32),
    ]
    scratch += [pltpu.VMEM((128, 128), F32)] * 5
    params = (wx, wb, wc, offset, fading)
    width = x_total + 2 * b.shape[1]
    early = [pltpu.VMEM((sp,) + one.shape, one.dtype) for one in params]
    early += [pltpu.VMEM((8, width), F32), pltpu.VMEM((8, 128), F32), pltpu.VMEM((8, width), F32)]
    early += [pltpu.VMEM((EDGE, one.shape[1]), BF16) for one in (x, b, c)] * 2
    early += [pltpu.SemaphoreType.DMA((2, 5, sp)), pltpu.SemaphoreType.DMA((2, 2, 3))]
    scratch += early
    split = 1
    for level in levels:
        split *= level[1]
    chunks = 2 if groups % (2 * split) == 0 else 1
    counts = [level[1] for level in levels] + [top[1]]
    scratch += [pltpu.VMEM((8, 128), F32)] * len(counts)
    scratch += [pltpu.VMEM((n, 8, 128), F32) for n in counts]
    scratch += [pltpu.VMEM((n, 128, 128), F32) for n in counts]
    scratch += [pltpu.SemaphoreType.DMA((2, n)) for n in counts]
    for _ in range(chunks):
        held = [x_total // chunks]
        for n in counts[:-1]:
            held.append(held[-1] // n)
        slabs = list(zip(counts[:-1], held[1:]))
        scratch += [pltpu.VMEM((2, rows, STATE), BF16) for rows in held]
        scratch += [pltpu.VMEM((n, 2, rows, STATE), BF16) for n, rows in slabs]
        scratch += [pltpu.VMEM((counts[-1], held[-1], STATE), BF16)]
        scratch += [pltpu.VMEM((2, rows, STATE), BF16) for rows in held[:-1]]
        scratch += [pltpu.VMEM((n, 2, rows, STATE), BF16) for n, rows in slabs]
        scratch += [pltpu.SemaphoreType.DMA((4, n)) for n in counts]
        scratch += [pltpu.VMEM((2, held[-1], STATE), F32)]
    out = pl.pallas_call(
        functools.partial(kernel, levels, top, (heads, pairs, chunks, sp, dp)),
        out_shape=jax.ShapeDtypeStruct((blk, x_total), BF16),
        in_specs=[pl.BlockSpec(memory_space=pltpu.VMEM)] * 13,
        out_specs=pl.BlockSpec(memory_space=pltpu.VMEM),
        scratch_shapes=scratch,
        compiler_params=pltpu.CompilerParams(
            collective_id=0, has_side_effects=True, vmem_limit_bytes=60 * 2**20
        ),
        name="mixer",
    )(x, b, c, z, ahead[0].T, back[0].T, spike[0].T, *params, gain.astype(F32)[None])
    return out[None]


def solution(mesh):
    tokens = P("dp", "sp", None)
    placed = (tokens,) * 7 + (P(None, "sp"),) * 5 + (P(),)
    return jax.shard_map(
        functools.partial(local, mesh.shape["sp"], mesh.shape["dp"]),
        mesh=mesh,
        in_specs=placed,
        out_specs=tokens,
        check_vma=False,
    )
```
